32 devices in a mesh: grp: 2 (over y), ep: 4 (over z), tp: 4 (over x, core).
Axes of the slice: x: 2, y: 2, z: 4, core: 2. Of those that a mesh axis runs over, the one named last changes fastest.
Arguments:
- queries: bfloat16 [1024, 2048], P(('grp', 'ep'), 'tp'), parts along dimension 0, may hold values from -6 to 6
- keys: bfloat16 [1024, 2048], P(('grp', 'ep'), 'tp'), parts along dimension 0, may hold values from -6 to 6
- values: bfloat16 [1024, 2048], P(('grp', 'ep'), 'tp'), parts along dimension 0, may hold values from -6 to 6
- stop_bias: bfloat16 [1024, 32], P(('grp', 'ep'), 'tp'), parts along dimension 0, may hold values from -20 to 0
- out_weight: bfloat16 [2048, 2048], P('tp'), may hold values from -0.125 to 0.125
- mix_gain: float32 [2048], replicated, may hold values from 0.1 to 1.9
- moe_input: bfloat16 [4096, 2048], P(('grp', 'ep', 'tp')), parts along dimension 0, may hold values from -6 to 6
- ffn_gain: float32 [2048], replicated, may hold values from 0.1 to 1.9
- expert_ids: int32 [4096, 2], P(('grp', 'ep', 'tp')), parts along dimension 0, may hold values from 0 to 3, all different within a row; in each aligned block of 128 rows (0 to 127, 128 to 255, ...) at most 96 rows name the same one
- expert_scores: float32 [4096, 2], P(('grp', 'ep', 'tp')), parts along dimension 0, may hold values from 0.05 to 1
- gate_weight: bfloat16 [4, 2048, 1024], P('ep', None, 'tp'), may hold values from -0.125 to 0.125
- up_weight: bfloat16 [4, 2048, 1024], P('ep', None, 'tp'), may hold values from -0.125 to 0.125
- down_weight: bfloat16 [4, 1024, 2048], P('ep', 'tp'), may hold values from -0.1875 to 0.1875
Outputs:
- mixed: bfloat16 [1024, 2048], P(('grp', 'ep', 'tp')), parts along dimension 0
- experts_mixed: bfloat16 [4096, 2048], P(('grp', 'ep', 'tp')), parts along dimension 0
The draws below stay inside these ranges and needn't reach their ends.
There are 2 independent parts, one for each index of `grp`. The reference program is written for one: setup_inputs(seed, part) draws one part's arguments, and reference() takes and returns one part's arrays. A program takes and returns all parts, laid end to end along the dimension named above; an argument that names none is the same for every part. Nothing has to cross between parts.
Inputs may be any that keep to these rules, and one draw needn't show every extreme that they name: `expert_ids`: each token names 2 different experts. Among the 128 tokens of one device, no expert is named by more than 96 tokens, and in some device's tokens some expert is named by exactly 96.
All inputs are finite; a program needn't handle non-finite values.
Results may differ from the reference program's by a relative error of at most 0.012.
Values may be sent and summed in bfloat16 or wider, within the bound.
A program may use at most 128 MiB of HBM per device.

```python
import math
import jax
import jax.numpy as jnp
import numpy as np
from jax import lax

D = 2048
HEADS = 32
HEAD = 64
FF = 1024
TOP_K = 2
SEQ_DEV = 128
TOK_DEV = 128
CONTEXT_LENGTH = 512
TOKENS = 2048
EXPERTS = 4
CAP = 96
N_EP = 4
N_TP = 4


def draw_stop_bias(key, part):
    streams = jax.random.split(key, 7)
    fast = jax.random.uniform(streams[0], (HEADS,)) < 0.5
    slow_rate = jax.random.uniform(streams[1], (HEADS,), minval=0.1, maxval=0.4) / CONTEXT_LENGTH
    fast_rate = jax.random.uniform(streams[2], (HEADS,), minval=1.0 / 150.0, maxval=1.0 / 60.0)
    starting_level = jnp.log(jnp.where(fast, fast_rate, slow_rate))
    displacement_delta = jax.random.uniform(streams[3], (CONTEXT_LENGTH // SEQ_DEV, 1), minval=-0.7, maxval=0.7)
    displacement_delta = jnp.repeat(displacement_delta, SEQ_DEV, axis=0)
    approximate_guess = jax.random.uniform(streams[4], (CONTEXT_LENGTH, HEADS), minval=-2.0, maxval=2.0)
    location_number = jax.random.randint(streams[5], (4,), 0, CONTEXT_LENGTH)
    spike_height = jnp.any(jnp.arange(CONTEXT_LENGTH)[:, None] == location_number[None, :], axis=1)
    intensity_multiplier = jax.random.uniform(streams[6], (CONTEXT_LENGTH, HEADS), minval=0.25, maxval=0.4)
    closing_answer = jnp.where(spike_height[:, None], jnp.log(intensity_multiplier / (1.0 - intensity_multiplier)), starting_level[None, :] + displacement_delta + approximate_guess)
    return closing_answer.astype(jnp.bfloat16)


def level_of(key, extent, cuts, low, largest):
    def one(position, blocks):
        heights = jax.random.uniform(jax.random.fold_in(jax.random.fold_in(key, 6), position), (blocks,), jnp.float32, low / len(cuts), largest / len(cuts))
        return jnp.repeat(jnp.exp(heights), extent[position] // blocks).reshape((-1,) + (1,) * (len(extent) - position - 1))

    loudness = one(*cuts[0])
    for cut in cuts[1:]:
        loudness = loudness * one(*cut)
    return loudness


def routed_block(stream_key, own, number, rows, amount, top, limit, slope):
    sequence = jax.random.permutation(stream_key, amount)
    heavy_load, usual = shares(amount, rows * top, limit, slope, True), shares(amount, rows * top, limit, slope, False)
    places = jnp.arange(amount)

    def named(tallies, turn):
        used = int((tallies > 0).sum())
        fixed = max(1, used // 4)
        shifted = fixed + (places - fixed + turn * (used - fixed)) % max(1, amount - fixed)
        return jnp.zeros((amount,), jnp.int32).at[sequence[jnp.where(places < fixed, places, shifted)]].set(jnp.asarray(tallies, jnp.int32))

    tallies = jnp.where(number % 4 == 0, named(heavy_load, number // 4), named(usual, number - number // 4 - 1))
    mixed = jax.random.permutation(jax.random.fold_in(own, 3), amount)
    giver, sink = mixed[0:amount // 2 * 2:2], mixed[1:amount // 2 * 2:2]
    margin = jnp.minimum(tallies[giver] - 1, limit - tallies[sink]) // 2
    margin = jnp.where((giver == sequence[0]) | (sink == sequence[0]) | (tallies[sink] == 0), 0, jnp.maximum(margin, 0))
    shifted = jax.random.randint(jax.random.fold_in(own, 4), (amount // 2,), 0, 1 << 20) % (margin + 1)
    tallies = tallies.at[giver].add(-shifted).at[sink].add(shifted)
    members = jnp.searchsorted(jnp.cumsum(tallies), jnp.arange(rows * top), side="right").astype(jnp.int32)
    table = members.reshape(top, rows).T
    table = table[jax.random.permutation(jax.random.fold_in(own, 1), rows)]
    turn = jax.random.randint(jax.random.fold_in(own, 2), (rows, 1), 0, top)
    return jnp.take_along_axis(table, (jnp.arange(top)[None, :] + turn) % top, axis=1)


def shares(number_of, total, bound, skew, full):
    loads = [(1 << 20) // math.isqrt(standing ** skew) + 1 for standing in range(1, number_of + 1)]
    largest = bound if full else min(bound, max(-(-total // number_of), total * loads[0] // sum(loads)))
    least = 1 if total - largest >= number_of - 1 else 0
    counts, spare = [largest] + [least] * (number_of - 1), total - largest - least * (number_of - 1)
    while spare > 0:
        candidates = [i for i in range(1, number_of) if counts[i] < largest] or [i for i in range(1, number_of) if counts[i] < bound]
        mass, remaining = sum([loads[i] for i in candidates]), spare
        for i in candidates:
            addition = min(bound - counts[i], max(1, remaining * loads[i] // mass), spare)
            counts[i] = counts[i] + addition
            spare = spare - addition
    return np.array(counts)


def scatter_about(own_key, shape, scale, bound, cuts=(), held_as=jnp.bfloat16):
    values = jax.random.normal(own_key, shape, jnp.float32) * scale
    if len(cuts) > 0:
        values = level_of(own_key, shape, cuts, -0.22, 0.18) * values
    return jnp.clip(values, min=-bound, max=bound).astype(held_as)


def setup_inputs(seed: int = 0, part: int = 0) -> dict:
    key_of = jax.random.split(jax.random.key(seed), 14)
    own_keys = jax.random.split(jax.random.fold_in(key_of[13], part), 14)
    queries = scatter_about(own_keys[0], (CONTEXT_LENGTH, HEADS * HEAD), 1.0, 6.0, ((0, 4), (1, 4)))
    keys = scatter_about(own_keys[1], (CONTEXT_LENGTH, HEADS * HEAD), 1.0, 6.0, ((0, 4), (1, 4)))
    values = scatter_about(own_keys[2], (CONTEXT_LENGTH, HEADS * HEAD), 1.0, 6.0, ((0, 4), (1, 4)))
    stop_bias = draw_stop_bias(jax.random.fold_in(jax.random.fold_in(key_of[13], part), 71), part)
    out_weight = scatter_about(key_of[4], (HEADS * HEAD, D), (HEADS * HEAD) ** -0.5, 0.125, ((0, 4),))
    mix_gain = jnp.clip(1.0 + 0.18 * jax.random.normal(key_of[5], (D,), jnp.float32), 0.1, 1.9)
    moe_input = scatter_about(own_keys[6], (TOKENS, D), 1.0, 6.0, ((0, 16),))
    ffn_gain = jnp.clip(1.0 + 0.18 * jax.random.normal(key_of[7], (D,), jnp.float32), 0.1, 1.9)
    expert_ids_keys = jax.random.split(jax.random.fold_in(own_keys[8], 1), TOKENS // TOK_DEV)
    expert_ids_turns = jax.random.permutation(jax.random.fold_in(own_keys[8], 3), TOKENS // TOK_DEV)
    expert_ids = jax.vmap(lambda own, number: routed_block(jax.random.fold_in(own_keys[8], 2), own, number, TOK_DEV, EXPERTS, TOP_K, CAP, 2))(expert_ids_keys, expert_ids_turns).reshape((TOKENS, TOP_K))
    expert_scores = jnp.clip(jnp.exp(math.log(1.0) - 2.9957323 * jax.random.uniform(own_keys[9], (TOKENS, TOP_K), jnp.float32) ** level_of(own_keys[9], (TOKENS, TOP_K), ((0, 16),), -0.2, 0.2)), 0.05, 1.0)
    gate_weight = scatter_about(key_of[10], (EXPERTS, D, FF), D ** -0.5, 0.125, ((0, 4), (2, 4)))
    up_weight = scatter_about(key_of[11], (EXPERTS, D, FF), D ** -0.5, 0.125, ((0, 4), (2, 4)))
    down_weight = scatter_about(key_of[12], (EXPERTS, FF, D), FF ** -0.5, 0.1875, ((0, 4), (1, 4)))
    return dict(queries=queries, keys=keys, values=values, stop_bias=stop_bias, out_weight=out_weight, mix_gain=mix_gain, moe_input=moe_input, ffn_gain=ffn_gain, expert_ids=expert_ids, expert_scores=expert_scores, gate_weight=gate_weight, up_weight=up_weight, down_weight=down_weight)


def norm_rows(values, gain):
    values = values.astype(jnp.float32)
    scale = lax.rsqrt(lax.optimization_barrier(jnp.mean(values * values, axis=-1, keepdims=True)) + 1e-06)
    return values * scale * gain

def settle(term):
    return lax.optimization_barrier(term.astype(jnp.bfloat16)).astype(jnp.float32)

def stick_head(inputs):
    query, key, value, bias = inputs
    length = query.shape[0]
    count = length // SEQ_DEV
    scores = jnp.dot(query, key.T, preferred_element_type=jnp.float32) * HEAD ** (-0.5)
    scores = scores + bias.astype(jnp.float32)[None, :]
    place = jnp.arange(length)
    past = place[None, :] < place[:, None]
    rest = jnp.where(past, jax.nn.log_sigmoid(-scores), 0.0)
    rest_blocks = rest.reshape(length, count, SEQ_DEV)
    later = lax.cumsum(rest_blocks, axis=2, reverse=True)
    within = (later - rest_blocks).reshape(length, length)
    totals = later[:, :, 0]
    local = jnp.where(past, jnp.exp(jax.nn.log_sigmoid(scores) + within), 0.0).astype(jnp.bfloat16)
    parts = jnp.einsum('tbs,bsd->tbd', local.reshape(length, count, SEQ_DEV).astype(jnp.float32), value.reshape(count, SEQ_DEV, HEAD).astype(jnp.float32), precision=lax.Precision.HIGHEST)
    carried = lax.cumsum(totals, axis=1, reverse=True) - totals
    return lax.optimization_barrier(jnp.sum(jnp.exp(carried)[:, :, None] * parts, axis=1))

def reference(queries, keys, values, stop_bias, out_weight, mix_gain, moe_input, ffn_gain, expert_ids, expert_scores, gate_weight, up_weight, down_weight):
    length = queries.shape[0]

    def by_head(array):
        return array.reshape(length, HEADS, HEAD).transpose(1, 0, 2)
    attended = lax.map(stick_head, (by_head(queries), by_head(keys), by_head(values), stop_bias.T))
    attended = attended.transpose(1, 0, 2).reshape(length, HEADS * HEAD).astype(jnp.bfloat16)
    group = HEADS * HEAD // N_TP
    projected = jnp.zeros((length, D), jnp.float32)
    for quarter in range(N_TP):
        term = jnp.dot(attended[:, quarter * group:(quarter + 1) * group], out_weight[quarter * group:(quarter + 1) * group], preferred_element_type=jnp.float32)
        projected = projected + settle(term)
    mixed = norm_rows(projected, mix_gain).astype(jnp.bfloat16)
    normed = norm_rows(moe_input, ffn_gain).astype(jnp.bfloat16)
    weights = expert_scores / lax.optimization_barrier(jnp.sum(expert_scores, axis=1, keepdims=True))
    load = N_EP * N_TP * CAP
    share = FF // N_TP

    def one_expert(total, expert):
        named = expert_ids == expert
        present = jnp.any(named, axis=1)
        weight = lax.optimization_barrier(jnp.sum(jnp.where(named, weights, 0.0), axis=1))
        chosen = jnp.nonzero(present, size=load, fill_value=0)[0].astype(jnp.int32)
        valid = jnp.arange(load) < jnp.sum(present.astype(jnp.int32))
        rows = normed[chosen]
        gate = jnp.dot(rows, gate_weight[expert], preferred_element_type=jnp.float32)
        upward = jnp.dot(rows, up_weight[expert], preferred_element_type=jnp.float32)
        hidden = (jax.nn.silu(gate) * upward).astype(jnp.bfloat16)
        lowering = down_weight[expert]
        summed = jnp.zeros((load, D), jnp.float32)
        for quarter in range(N_TP):
            term = jnp.dot(hidden[:, quarter * share:(quarter + 1) * share], lowering[quarter * share:(quarter + 1) * share], preferred_element_type=jnp.float32)
            summed = summed + settle(term)
        output = settle(summed)
        contribution = jnp.where(valid[:, None], weight[chosen][:, None] * output, 0.0)
        return (total.at[chosen].add(contribution), None)
    total, _ = lax.scan(one_expert, jnp.zeros((TOKENS, D), jnp.float32), jnp.arange(EXPERTS, dtype=jnp.int32))
    return (mixed, total.astype(jnp.bfloat16))
```

```python
import functools

import jax
import jax.numpy as jnp
from jax import lax
from jax.experimental import pallas as pl
from jax.experimental.pallas import tpu as pltpu
from jax.sharding import PartitionSpec as P

MESH = pl.DeviceIdType.MESH
F32 = jnp.float32
BF16 = jnp.bfloat16


def norm_rows(values, gain):
    values = values.astype(jnp.float32)
    scale = lax.rsqrt(jnp.mean(values * values, axis=-1, keepdims=True) + 1e-06)
    return values * scale * gain


def break_terms(query_heads, query_place, key_block, bias_block, first):
    span = key_block.shape[0]
    heads = query_heads.shape[1]
    key_heads = key_block.reshape(span, heads, -1)
    scores = jnp.einsum("qhd,khd->hqk", query_heads, key_heads, preferred_element_type=jnp.float32)
    scores = scores * query_heads.shape[2] ** (-0.5) + bias_block.astype(jnp.float32).T[:, None, :]
    key_place = first + jnp.arange(span)
    past = (key_place[None, :] < query_place[:, None])[None]
    rest = jnp.where(past, jax.nn.log_sigmoid(-scores), 0.0)
    later = lax.cumsum(rest, axis=2, reverse=True)
    return (scores, past, rest, later)


def block_part(scores, past, rest, later, value_block, heads):
    within = later - rest
    local = jnp.where(past, jnp.exp(jax.nn.log_sigmoid(scores) + within), 0.0).astype(jnp.bfloat16)
    span = value_block.shape[0]
    value_heads = value_block.reshape(span, heads, -1)
    part = jnp.einsum("hqk,khd->qhd", local, value_heads, preferred_element_type=jnp.float32)
    return part.reshape(part.shape[0], -1)


def keep(state):
    return state


def dispatch_plan(normed, expert_ids, experts, capacity):
    rows, top = expert_ids.shape
    flat_ids = expert_ids.reshape(rows * top)
    onehot = (flat_ids[:, None] == jnp.arange(experts)[None, :]).astype(jnp.int32)
    earlier = jnp.cumsum(onehot, axis=0) - onehot
    place = jnp.sum(earlier * onehot, axis=1)
    target = flat_ids * capacity + place
    source = (
        jnp.zeros((experts * capacity,), jnp.int32)
        .at[target]
        .set(jnp.arange(rows * top, dtype=jnp.int32) // top + 1)
    )
    padded = jnp.concatenate([jnp.zeros((1, normed.shape[1]), normed.dtype), normed], axis=0)
    return (padded[source].reshape(experts, capacity, normed.shape[1]), target)


def expert_hidden(piece, gate_weight, up_weight):
    flat = piece.reshape(-1, piece.shape[-1])
    gate = jnp.dot(flat, gate_weight[0], preferred_element_type=jnp.float32)
    upward = jnp.dot(flat, up_weight[0], preferred_element_type=jnp.float32)
    hidden = (jax.nn.silu(gate) * upward).astype(jnp.bfloat16)
    return hidden.reshape(piece.shape[0], piece.shape[1], -1)


def send_back(summed):
    return lax.all_to_all(
        summed.astype(jnp.bfloat16), "ep", split_axis=0, concat_axis=0, tiled=True
    )


def return_rows(hidden_all, down_weight, sources):
    flat = hidden_all.reshape(-1, hidden_all.shape[2])
    product = jnp.dot(flat, down_weight[0], preferred_element_type=jnp.float32)
    return send_back(
        lax.psum_scatter(
            product.reshape(sources * lax.axis_size("tp"), hidden_all.shape[1], -1).astype(
                jnp.bfloat16
            ),
            "tp",
            scatter_dimension=0,
            tiled=True,
        ).astype(jnp.float32)
    )


def per_device(
    queries,
    keys,
    values,
    stop_bias,
    out_weight,
    mix_gain,
    moe_input,
    ffn_gain,
    expert_ids,
    expert_scores,
    gate_weight,
    up_weight,
    down_weight,
):
    span = queries.shape[0]
    heads = stop_bias.shape[1]
    width_heads = queries.shape[1]
    blocks = lax.axis_size("ep")
    own_first = lax.axis_index("ep") * span
    query_heads = queries.reshape(span, heads, -1)
    query_place = own_first + jnp.arange(span)

    def piece_rows(piece, index):
        return tuple((lax.dynamic_slice_in_dim(member, index * span, span, 0) for member in piece))

    start_state = (
        jnp.zeros((blocks, heads, span), jnp.float32),
        jnp.zeros((blocks, span, width_heads), jnp.float32),
    )
    piece = (
        lax.all_gather(keys, "ep", axis=0, tiled=True),
        lax.all_gather(values, "ep", axis=0, tiled=True),
        lax.all_gather(stop_bias, "ep", axis=0, tiled=True),
    )

    def one_block(index, state):
        key_block, value_block, bias_block = piece_rows(piece, index)
        first = index * span

        def compute(inner_state):
            totals, parts = inner_state
            scores, past, rest, later = break_terms(
                query_heads, query_place, key_block, bias_block, first
            )
            part = block_part(scores, past, rest, later, value_block, heads)
            number = first // span
            totals = lax.dynamic_update_index_in_dim(totals, later[:, :, 0], number, 0)
            parts = lax.dynamic_update_index_in_dim(parts, part, number, 0)
            return (totals, parts)

        return lax.cond(first <= own_first, compute, keep, state)

    totals, parts = lax.fori_loop(0, piece[0].shape[0] // span, one_block, start_state)
    carried = lax.cumsum(totals, axis=0, reverse=True) - totals
    factor = jnp.exp(carried).transpose(0, 2, 1)[:, :, :, None]
    attended = jnp.sum(factor * parts.reshape(blocks, span, heads, -1), axis=0).reshape(
        span, width_heads
    )
    attended = attended.astype(jnp.bfloat16)
    projected = lax.psum_scatter(
        jnp.dot(attended, out_weight, preferred_element_type=jnp.float32).astype(jnp.bfloat16),
        "tp",
        scatter_dimension=0,
        tiled=True,
    ).astype(jnp.float32)
    mixed = norm_rows(projected, mix_gain).astype(jnp.bfloat16)
    normed = norm_rows(moe_input, ffn_gain).astype(jnp.bfloat16)
    rows, top = expert_ids.shape
    experts = lax.axis_size("ep")
    capacity = 3 * rows * top // (2 * experts)
    weights = expert_scores / jnp.sum(expert_scores, axis=1, keepdims=True)
    outbound, target = dispatch_plan(normed, expert_ids, experts, capacity)
    arrived = lax.all_to_all(outbound, "ep", split_axis=0, concat_axis=0, tiled=True)
    hidden_all = expert_hidden(
        lax.all_gather(arrived, "tp", axis=0, tiled=True), gate_weight, up_weight
    )
    returned = return_rows(hidden_all, down_weight, arrived.shape[0])
    picked = returned.reshape(experts * capacity, -1)[target].reshape(rows, top, -1)
    experts_mixed = jnp.sum(picked.astype(jnp.float32) * weights[:, :, None], axis=1).astype(
        jnp.bfloat16
    )
    return (mixed, experts_mixed)


def contract_rows(left, right):
    return lax.dot_general(left, right, (((0,), (0,)), ((), ())), preferred_element_type=F32)


def layer_kernel(
    ep,
    capacity,
    head,
    q_ref,
    k_ref,
    v_ref,
    bias_ref,
    ow_ref,
    mix_gain_ref,
    x_ref,
    ffn_gain_ref,
    ids_ref,
    scores_ref,
    g_ref,
    u_ref,
    d_ref,
    mixed_ref,
    out_ref,
    q_all,
    k_all,
    v_all,
    bias_all,
    att_send,
    att_all,
    proj,
    proj_in,
    sel,
    outbound,
    rows_in,
    acc,
    back_out,
    back_in,
    g_far,
    u_far,
    d_far,
    pack_send,
    pack_recv,
    row_send,
    row_recv,
    att_ssem,
    att_rsem,
    back_ssem,
    back_rsem,
    proj_ssem,
    proj_rsem,
    near_send,
    near_recv,
    x_send,
    x_recv,
    y_send,
    y_recv,
    fwd_send,
    fwd_recv,
):
    me = lax.axis_index("ep")
    tp = lax.axis_index("tp")
    grp = lax.axis_index("grp")
    chip, core = tp // 2, tp % 2
    mates = [None, chip * 2 + (1 - core), (1 - chip) * 2 + core, (1 - chip) * 2 + (1 - core)]
    span = q_ref.shape[0]
    width = q_all.shape[2]
    heads = width // head

    barrier = pltpu.get_barrier_semaphore()
    peers = [{"ep": lax.rem(me + r, ep)} for r in range(1, ep)]
    peers += [{"tp": mates[m]} for m in (1, 2, 3)] + [{"grp": 1 - grp}]
    for peer in peers:
        pl.semaphore_signal(barrier, inc=1, device_id=peer, device_id_type=MESH)
    pl.semaphore_wait(barrier, len(peers))

    def send(src, dst, ssem, rsem, peer):
        return pltpu.make_async_remote_copy(
            src_ref=src,
            dst_ref=dst,
            send_sem=ssem,
            recv_sem=rsem,
            device_id=peer,
            device_id_type=MESH,
        )

    weights = (g_ref, u_ref, d_ref)
    fars = (g_far, u_far, d_far)
    started = []

    def go(copy):
        copy.start()
        started.append(copy)
        return copy

    chunks = [(c, a) for c in range(g_ref.shape[1]) for a in range(3)]
    over_x = {}
    for n, (c, a) in enumerate(chunks):
        over_x[n] = go(
            send(
                weights[a].at[grp, c],
                fars[a].at[1, grp, c],
                x_send.at[n],
                x_recv.at[n],
                {"tp": mates[2]},
            )
        )
    near = [
        go(
            send(
                weights[a], fars[a].at[0], near_send.at[a], near_recv.at[a], {"tp": mates[1]}
            )
        )
        for a in range(3)
    ]
    packs = {}
    for r in (2, 1, 3)[: ep - 1]:
        dest = lax.rem(me + r, ep)
        cols = pl.ds(pl.multiple_of(dest * width, width), width)
        pieces = (
            (q_ref.at[:, cols], q_all.at[me]),
            (k_ref.at[:, cols], k_all.at[me]),
            (v_ref.at[:, cols], v_all.at[me]),
            (bias_ref.at[dest], bias_all.at[me]),
        )
        packs[r] = [
            go(send(s, t, pack_send.at[r, n], pack_recv.at[r, n], {"ep": dest}))
            for n, (s, t) in enumerate(pieces)
        ]
    values = x_ref[...].astype(F32)
    scale = lax.rsqrt(jnp.mean(values * values, axis=-1, keepdims=True) + 1e-06)
    normed = (values * scale * ffn_gain_ref[...]).astype(BF16)
    tokens = x_ref.shape[0]
    ids = ids_ref[...]
    square = (tokens, tokens)
    lane = lax.broadcasted_iota(jnp.int32, square, 1)
    sub = lax.broadcasted_iota(jnp.int32, square, 0)
    named = jnp.zeros(square, F32)
    for r in range(ep):
        e = lax.rem(me + r, ep)
        hit = jnp.max((ids == e).astype(F32), axis=1, keepdims=True)
        named = named + jnp.where(lane == r, hit, 0.0)
    named = named.astype(BF16)
    place = contract_rows(named, (sub < lane).astype(BF16))
    present = contract_rows(named, (sub == lane).astype(BF16))
    slot = lax.broadcasted_iota(jnp.int32, (capacity, tokens), 0).astype(F32)
    rows = {}
    for r in (2, 1, 3, 0):
        chosen = jnp.where(
            slot == place[r : r + 1, :], present[r : r + 1, :], 0.0
        ).astype(BF16)
        sel[r] = chosen
        picked = jnp.dot(chosen, normed, preferred_element_type=F32).astype(BF16)
        if r == 0:
            rows_in[0] = picked
        else:
            outbound[r] = picked
            rows[r] = go(
                send(
                    outbound.at[r],
                    rows_in.at[r],
                    row_send.at[r],
                    row_recv.at[r],
                    {"ep": lax.rem(me + r, ep)},
                )
            )
    own = pl.ds(pl.multiple_of(me * width, width), width)
    q_all[me] = q_ref[:, own]
    k_all[me] = k_ref[:, own]
    v_all[me] = v_ref[:, own]
    bias_all[me] = bias_ref[me]

    over_y, cross = {}, {}

    def forward(n):
        c, a = chunks[n]
        over_x[n].wait_recv()
        over_y[n] = go(
            send(
                fars[a].at[1, grp, c],
                fars[a].at[1, grp, c],
                y_send.at[n],
                y_recv.at[n],
                {"grp": 1 - grp},
            )
        )
        cross[0, n] = go(
            send(
                fars[a].at[1, grp, c],
                fars[a].at[2, grp, c],
                fwd_send.at[0, n],
                fwd_recv.at[0, n],
                {"tp": mates[1]},
            )
        )

    def forward_again(n):
        c, a = chunks[n]
        over_y[n].wait_recv()
        cross[1, n] = go(
            send(
                fars[a].at[1, 1 - grp, c],
                fars[a].at[2, 1 - grp, c],
                fwd_send.at[1, n],
                fwd_recv.at[1, n],
                {"tp": mates[1]},
            )
        )

    forward(0)
    for r in packs:
        for copy in packs[r]:
            copy.wait_recv()

    block = (span, span)
    key_sub = lax.broadcasted_iota(jnp.int32, block, 0)
    key_lane = lax.broadcasted_iota(jnp.int32, block, 1)
    after = (key_sub > key_lane).astype(BF16)

    def attend(i):
        def one(step, state):
            j = i - step
            past = (j * span + key_lane) < (i * span + key_sub)
            result = []
            for h in range(heads):
                total, carry = state[2 * h], state[2 * h + 1]
                cols = slice(h * head, (h + 1) * head)
                z = lax.dot_general(
                    q_all[i][:, cols],
                    k_all[j][:, cols],
                    (((1,), (1,)), ((), ())),
                    preferred_element_type=F32,
                )
                z = z * head ** (-0.5) + bias_all[j][h : h + 1, :]
                soft = jnp.log1p(jnp.exp(-jnp.abs(z)))
                stay = -(jnp.maximum(z, 0.0) + soft)
                stop = jnp.minimum(z, 0.0) - soft
                rest = jnp.where(past, stay, 0.0)
                hi = rest.astype(BF16)
                left = rest - hi.astype(F32)
                mid = left.astype(BF16)
                low = (left - mid.astype(F32)).astype(BF16)
                stack = jnp.concatenate([hi, mid, low], axis=0)
                sums = jnp.dot(stack, after, preferred_element_type=F32)
                within = sums[:span] + sums[span : 2 * span] + sums[2 * span :]
                local = jnp.where(past, jnp.exp(stop + within), 0.0).astype(BF16)
                part = jnp.dot(local, v_all[j][:, cols], preferred_element_type=F32)
                total = total + jnp.exp(carry) * part
                carry = carry + jnp.sum(rest, axis=1, keepdims=True)
                result += [total, carry]
            return tuple(result)

        start = (jnp.zeros((span, head), F32), jnp.zeros((span, 1), F32)) * heads
        state = lax.fori_loop(0, i + 1, one, start)
        return jnp.concatenate([state[2 * h] for h in range(heads)], axis=1).astype(BF16)

    att = {}
    pending = list(range(1, len(chunks)))
    for r in (2, 1, 3, 0):
        dest = lax.rem(me + r, ep)
        got = attend(dest)
        if r == 0:
            att_all[me] = got
        else:
            att_send[r] = got
            att[r] = go(
                send(att_send.at[r], att_all.at[me], att_ssem.at[r], att_rsem.at[r], {"ep": dest})
            )
        if pending:
            forward(pending.pop(0))
    for copy in near:
        copy.wait_recv()
    again = 0
    while pending:
        forward(pending.pop(0))
        forward_again(again)
        again += 1

    for r in rows:
        rows[r].wait_recv()
    deep = rows_in.shape[2]

    def hidden(g, u):
        flat = rows_in[...].reshape(ep * capacity, deep)
        gate = jnp.dot(flat, g.reshape(deep, -1), preferred_element_type=F32)
        up = jnp.dot(flat, u.reshape(deep, -1), preferred_element_type=F32)
        return (gate / (1.0 + jnp.exp(-gate)) * up).astype(BF16)

    def lower(h, d):
        return jnp.dot(h, d.reshape(-1, deep), preferred_element_type=F32)

    acc[...] = lower(hidden(g_ref[...], u_ref[...]), d_ref[...])
    acc[...] += lower(hidden(g_far[0], u_far[0]), d_far[0])
    while again < len(chunks):
        forward_again(again)
        again += 1
    acc[...] += lower(hidden(g_far[1], u_far[1]), d_far[1])
    for n in range(len(chunks)):
        cross[0, n].wait_recv()
        cross[1, n].wait_recv()
    last = hidden(g_far[2], u_far[2])
    back = {}
    for r in (2, 1, 3, 0):
        piece = slice(r * capacity, (r + 1) * capacity)
        final = (acc[piece, :] + lower(last[piece], d_far[2])).astype(BF16)
        if r == 0:
            back_in[0] = final
        else:
            back_out[r] = final
            back[r] = go(
                send(
                    back_out.at[r],
                    back_in.at[r],
                    back_ssem.at[r],
                    back_rsem.at[r],
                    {"ep": lax.rem(me + ep - r, ep)},
                )
            )
    for r in att:
        att[r].wait_recv()
    attended = jnp.concatenate([att_all[j] for j in range(ep)], axis=1)
    share = mixed_ref.shape[0]
    term = jnp.dot(attended, ow_ref[...], preferred_element_type=F32).astype(BF16)
    proj[...] = term.reshape(proj.shape)
    shares = [
        go(send(proj.at[mates[m]], proj_in.at[m], proj_ssem.at[m], proj_rsem.at[m], {"tp": mates[m]}))
        for m in (2, 3, 1)
    ]
    whole = proj[tp].astype(F32)
    for copy in shares:
        copy.wait_recv()
    for m in (1, 2, 3):
        whole = whole + proj_in[m].astype(F32)
    scale = lax.rsqrt(jnp.mean(whole * whole, axis=-1, keepdims=True) + 1e-06)
    mixed_ref[...] = (whole * scale * mix_gain_ref[...]).astype(BF16)
    scores = scores_ref[...]
    gates = scores / jnp.sum(scores, axis=1, keepdims=True)
    result = jnp.zeros((tokens, deep), F32)
    for r in (0, 1, 3, 2):
        if r:
            back[r].wait_recv()
        e = lax.rem(me + r, ep)
        weight = jnp.sum(jnp.where(ids == e, gates, 0.0), axis=1, keepdims=True)
        result = result + weight * contract_rows(sel[r], back_in[r])
    out_ref[...] = result.astype(BF16)
    for copy in started:
        copy.wait_send()


def fused_device(
    groups,
    ep,
    tp,
    queries,
    keys,
    values,
    stop_bias,
    out_weight,
    mix_gain,
    moe_input,
    ffn_gain,
    expert_ids,
    expert_scores,
    gate_weight,
    up_weight,
    down_weight,
):
    span, cols = queries.shape
    tokens, deep = moe_input.shape
    top = expert_ids.shape[1]
    capacity = 3 * tokens * top // (2 * ep)
    width = cols // ep
    heads = stop_bias.shape[1]
    own_heads = heads // ep
    units = gate_weight.shape[2]
    cuts = 2
    bias = stop_bias.T.astype(F32).reshape(ep, own_heads, span)
    bias = jnp.pad(bias, ((0, 0), (0, -own_heads % 8), (0, 0)))
    gate = gate_weight.reshape(groups, cuts, deep // (groups * cuts), units)
    up = up_weight.reshape(gate.shape)
    down = down_weight.reshape(groups, cuts, units // (groups * cuts), deep)
    chunks = 3 * cuts
    vmem = pl.BlockSpec(memory_space=pltpu.VMEM)
    dma = pltpu.SemaphoreType.DMA
    return pl.pallas_call(
        functools.partial(layer_kernel, ep, capacity, cols // heads),
        out_shape=(
            jax.ShapeDtypeStruct((span // tp, deep), BF16),
            jax.ShapeDtypeStruct((tokens, deep), BF16),
        ),
        in_specs=[vmem] * 13,
        out_specs=(vmem, vmem),
        scratch_shapes=[
            pltpu.VMEM((ep, span, width), BF16),
            pltpu.VMEM((ep, span, width), BF16),
            pltpu.VMEM((ep, span, width), BF16),
            pltpu.VMEM((ep,) + bias.shape[1:], F32),
            pltpu.VMEM((ep, span, width), BF16),
            pltpu.VMEM((ep, span, width), BF16),
            pltpu.VMEM((tp, span // tp, deep), BF16),
            pltpu.VMEM((tp, span // tp, deep), BF16),
            pltpu.VMEM((ep, capacity, tokens), BF16),
            pltpu.VMEM((ep, capacity, deep), BF16),
            pltpu.VMEM((ep, capacity, deep), BF16),
            pltpu.VMEM((ep * capacity, deep), F32),
            pltpu.VMEM((ep, capacity, deep), BF16),
            pltpu.VMEM((ep, capacity, deep), BF16),
            pltpu.VMEM((3,) + gate.shape, BF16),
            pltpu.VMEM((3,) + up.shape, BF16),
            pltpu.VMEM((3,) + down.shape, BF16),
            dma((ep, 4)),
            dma((ep, 4)),
            dma((ep,)),
            dma((ep,)),
            dma((ep,)),
            dma((ep,)),
            dma((ep,)),
            dma((ep,)),
            dma((tp,)),
            dma((tp,)),
            dma((3,)),
            dma((3,)),
            dma((chunks,)),
            dma((chunks,)),
            dma((chunks,)),
            dma((chunks,)),
            dma((2, chunks)),
            dma((2, chunks)),
        ],
        compiler_params=pltpu.CompilerParams(
            collective_id=0, has_side_effects=True, vmem_limit_bytes=60 * 2**20
        ),
    )(
        queries,
        keys,
        values,
        bias,
        out_weight,
        mix_gain.reshape(1, deep),
        moe_input,
        ffn_gain.reshape(1, deep),
        expert_ids,
        expert_scores,
        gate,
        up,
        down,
    )


def pick_plan(groups, ep, tp, *args):
    heads = args[3].shape[1]
    width = args[0].shape[1] // ep
    if groups == 2 and tp == 4 and ep == 4 and heads % ep == 0 and width % 128 == 0:
        return fused_device(groups, ep, tp, *args)
    return per_device(*args)


def solution(mesh):
    return jax.shard_map(
        functools.partial(pick_plan, mesh.shape["grp"], mesh.shape["ep"], mesh.shape["tp"]),
        mesh=mesh,
        in_specs=(
            P(("grp", "ep"), "tp"),
            P(("grp", "ep"), "tp"),
            P(("grp", "ep"), "tp"),
            P(("grp", "ep"), "tp"),
            P("tp", None),
            P(),
            P(("grp", "ep", "tp"), None),
            P(),
            P(("grp", "ep", "tp"), None),
            P(("grp", "ep", "tp"), None),
            P("ep", None, "tp"),
            P("ep", None, "tp"),
            P("ep", "tp", None),
        ),
        out_specs=(P(("grp", "ep", "tp"), None), P(("grp", "ep", "tp"), None)),
        check_vma=False,
    )
```

```python
import functools

import jax
import jax.numpy as jnp
from jax import lax
from jax.experimental import pallas as pl
from jax.experimental.pallas import tpu as pltpu
from jax.sharding import PartitionSpec as P

MESH = pl.DeviceIdType.MESH
F32 = jnp.float32
BF16 = jnp.bfloat16


def norm_rows(values, gain):
    values = values.astype(jnp.float32)
    scale = lax.rsqrt(jnp.mean(values * values, axis=-1, keepdims=True) + 1e-06)
    return values * scale * gain


def break_terms(query_heads, query_place, key_block, bias_block, first):
    span = key_block.shape[0]
    heads = query_heads.shape[1]
    key_heads = key_block.reshape(span, heads, -1)
    scores = jnp.einsum("qhd,khd->hqk", query_heads, key_heads, preferred_element_type=jnp.float32)
    scores = scores * query_heads.shape[2] ** (-0.5) + bias_block.astype(jnp.float32).T[:, None, :]
    key_place = first + jnp.arange(span)
    past = (key_place[None, :] < query_place[:, None])[None]
    rest = jnp.where(past, jax.nn.log_sigmoid(-scores), 0.0)
    later = lax.cumsum(rest, axis=2, reverse=True)
    return (scores, past, rest, later)


def block_part(scores, past, rest, later, value_block, heads):
    within = later - rest
    local = jnp.where(past, jnp.exp(jax.nn.log_sigmoid(scores) + within), 0.0).astype(jnp.bfloat16)
    span = value_block.shape[0]
    value_heads = value_block.reshape(span, heads, -1)
    part = jnp.einsum("hqk,khd->qhd", local, value_heads, preferred_element_type=jnp.float32)
    return part.reshape(part.shape[0], -1)


def keep(state):
    return state


def dispatch_plan(normed, expert_ids, experts, capacity):
    rows, top = expert_ids.shape
    flat_ids = expert_ids.reshape(rows * top)
    onehot = (flat_ids[:, None] == jnp.arange(experts)[None, :]).astype(jnp.int32)
    earlier = jnp.cumsum(onehot, axis=0) - onehot
    place = jnp.sum(earlier * onehot, axis=1)
    target = flat_ids * capacity + place
    source = (
        jnp.zeros((experts * capacity,), jnp.int32)
        .at[target]
        .set(jnp.arange(rows * top, dtype=jnp.int32) // top + 1)
    )
    padded = jnp.concatenate([jnp.zeros((1, normed.shape[1]), normed.dtype), normed], axis=0)
    return (padded[source].reshape(experts, capacity, normed.shape[1]), target)


def expert_hidden(piece, gate_weight, up_weight):
    flat = piece.reshape(-1, piece.shape[-1])
    gate = jnp.dot(flat, gate_weight[0], preferred_element_type=jnp.float32)
    upward = jnp.dot(flat, up_weight[0], preferred_element_type=jnp.float32)
    hidden = (jax.nn.silu(gate) * upward).astype(jnp.bfloat16)
    return hidden.reshape(piece.shape[0], piece.shape[1], -1)


def send_back(summed):
    return lax.all_to_all(
        summed.astype(jnp.bfloat16), "ep", split_axis=0, concat_axis=0, tiled=True
    )


def return_rows(hidden_all, down_weight, sources):
    flat = hidden_all.reshape(-1, hidden_all.shape[2])
    product = jnp.dot(flat, down_weight[0], preferred_element_type=jnp.float32)
    return send_back(
        lax.psum_scatter(
            product.reshape(sources * lax.axis_size("tp"), hidden_all.shape[1], -1).astype(
                jnp.bfloat16
            ),
            "tp",
            scatter_dimension=0,
            tiled=True,
        ).astype(jnp.float32)
    )


def per_device(
    queries,
    keys,
    values,
    stop_bias,
    out_weight,
    mix_gain,
    moe_input,
    ffn_gain,
    expert_ids,
    expert_scores,
    gate_weight,
    up_weight,
    down_weight,
):
    span = queries.shape[0]
    heads = stop_bias.shape[1]
    width_heads = queries.shape[1]
    blocks = lax.axis_size("ep")
    own_first = lax.axis_index("ep") * span
    query_heads = queries.reshape(span, heads, -1)
    query_place = own_first + jnp.arange(span)

    def piece_rows(piece, index):
        return tuple((lax.dynamic_slice_in_dim(member, index * span, span, 0) for member in piece))

    start_state = (
        jnp.zeros((blocks, heads, span), jnp.float32),
        jnp.zeros((blocks, span, width_heads), jnp.float32),
    )
    piece = (
        lax.all_gather(keys, "ep", axis=0, tiled=True),
        lax.all_gather(values, "ep", axis=0, tiled=True),
        lax.all_gather(stop_bias, "ep", axis=0, tiled=True),
    )

    def one_block(index, state):
        key_block, value_block, bias_block = piece_rows(piece, index)
        first = index * span

        def compute(inner_state):
            totals, parts = inner_state
            scores, past, rest, later = break_terms(
                query_heads, query_place, key_block, bias_block, first
            )
            part = block_part(scores, past, rest, later, value_block, heads)
            number = first // span
            totals = lax.dynamic_update_index_in_dim(totals, later[:, :, 0], number, 0)
            parts = lax.dynamic_update_index_in_dim(parts, part, number, 0)
            return (totals, parts)

        return lax.cond(first <= own_first, compute, keep, state)

    totals, parts = lax.fori_loop(0, piece[0].shape[0] // span, one_block, start_state)
    carried = lax.cumsum(totals, axis=0, reverse=True) - totals
    factor = jnp.exp(carried).transpose(0, 2, 1)[:, :, :, None]
    attended = jnp.sum(factor * parts.reshape(blocks, span, heads, -1), axis=0).reshape(
        span, width_heads
    )
    attended = attended.astype(jnp.bfloat16)
    projected = lax.psum_scatter(
        jnp.dot(attended, out_weight, preferred_element_type=jnp.float32).astype(jnp.bfloat16),
        "tp",
        scatter_dimension=0,
        tiled=True,
    ).astype(jnp.float32)
    mixed = norm_rows(projected, mix_gain).astype(jnp.bfloat16)
    normed = norm_rows(moe_input, ffn_gain).astype(jnp.bfloat16)
    rows, top = expert_ids.shape
    experts = lax.axis_size("ep")
    capacity = 3 * rows * top // (2 * experts)
    weights = expert_scores / jnp.sum(expert_scores, axis=1, keepdims=True)
    outbound, target = dispatch_plan(normed, expert_ids, experts, capacity)
    arrived = lax.all_to_all(outbound, "ep", split_axis=0, concat_axis=0, tiled=True)
    hidden_all = expert_hidden(
        lax.all_gather(arrived, "tp", axis=0, tiled=True), gate_weight, up_weight
    )
    returned = return_rows(hidden_all, down_weight, arrived.shape[0])
    picked = returned.reshape(experts * capacity, -1)[target].reshape(rows, top, -1)
    experts_mixed = jnp.sum(picked.astype(jnp.float32) * weights[:, :, None], axis=1).astype(
        jnp.bfloat16
    )
    return (mixed, experts_mixed)


def contract_rows(left, right):
    return lax.dot_general(left, right, (((0,), (0,)), ((), ())), preferred_element_type=F32)


def layer_kernel(
    ep,
    capacity,
    head,
    q_ref,
    k_ref,
    v_ref,
    bias_ref,
    ow_ref,
    mix_gain_ref,
    x_ref,
    ffn_gain_ref,
    ids_ref,
    scores_ref,
    g_ref,
    u_ref,
    d_ref,
    mixed_ref,
    out_ref,
    q_all,
    k_all,
    v_all,
    bias_all,
    bias_rows,
    att_send,
    att_all,
    proj,
    proj_in,
    ow,
    meta,
    meta_in,
    normed_ref,
    dense_in,
    sel,
    gate_cols,
    outbound,
    relay_out,
    rows_in,
    acc,
    back_out,
    back_in,
    outer_out,
    outer_in,
    dense_out,
    dense_back,
    g_far,
    u_far,
    d_far,
    ow_sem,
    pack_send,
    pack_recv,
    row_send,
    row_recv,
    meta_send,
    meta_recv,
    dense_send,
    dense_recv,
    relay_send,
    relay_recv,
    att_ssem,
    att_rsem,
    back_ssem,
    back_rsem,
    outer_send,
    outer_recv,
    home_send,
    home_recv,
    proj_ssem,
    proj_rsem,
    near_send,
    near_recv,
    x_send,
    x_recv,
    y_send,
    y_recv,
    fwd_send,
    fwd_recv,
):
    me = lax.axis_index("ep")
    tp = lax.axis_index("tp")
    grp = lax.axis_index("grp")
    chip, core = tp // 2, tp % 2
    mates = [None, chip * 2 + (1 - core), (1 - chip) * 2 + core, (1 - chip) * 2 + (1 - core)]
    span = q_ref.shape[0]
    width = q_all.shape[2]
    heads = width // head

    half = me // 2
    inner = lax.rem(me + 1, ep) >= 2
    side = me + 1 - 2 * (me % 2)
    far_inner = 2 - half
    far_base = 2 * (1 - half)
    ow_copy = pltpu.make_async_copy(ow_ref, ow, ow_sem)
    ow_copy.start()

    barrier = pltpu.get_barrier_semaphore()
    peers = [{"ep": lax.rem(me + r, ep)} for r in range(1, ep)]
    peers += [{"tp": mates[m]} for m in (1, 2, 3)] + [{"grp": 1 - grp}]
    for peer in peers:
        pl.semaphore_signal(barrier, inc=1, device_id=peer, device_id_type=MESH)
    pl.semaphore_wait(barrier, len(peers))

    def send(src, dst, ssem, rsem, peer):
        return pltpu.make_async_remote_copy(
            src_ref=src,
            dst_ref=dst,
            send_sem=ssem,
            recv_sem=rsem,
            device_id=peer,
            device_id_type=MESH,
        )

    weights = (g_ref, u_ref, d_ref)
    fars = (g_far, u_far, d_far)
    started = []

    def go(copy):
        copy.start()
        started.append(copy)
        return copy

    cuts = g_ref.shape[1]
    chunks = [(c, a) for c in range(cuts) for a in range(2)] + [(c, 2) for c in range(cuts)]
    over_x = {}
    for n, (c, a) in enumerate(chunks):
        over_x[n] = go(
            send(
                weights[a].at[grp, c],
                fars[a].at[1, grp, c],
                x_send.at[n],
                x_recv.at[n],
                {"tp": mates[2]},
            )
        )
    near = [
        go(
            send(
                weights[a], fars[a].at[0], near_send.at[a], near_recv.at[a], {"tp": mates[1]}
            )
        )
        for a in range(3)
    ]
    packs = {}
    for r in (2, 1, 3)[: ep - 1]:
        dest = lax.rem(me + r, ep)
        cols = pl.ds(pl.multiple_of(dest * width, width), width)
        pieces = (
            (q_ref.at[:, cols], q_all.at[me]),
            (k_ref.at[:, cols], k_all.at[me]),
            (v_ref.at[:, cols], v_all.at[me]),
            (bias_ref, bias_all.at[me]),
        )
        packs[r] = [
            go(send(s, t, pack_send.at[r, n], pack_recv.at[r, n], {"ep": dest}))
            for n, (s, t) in enumerate(pieces)
        ]
    tokens, deep = x_ref.shape
    top = ids_ref.shape[0]
    scores = scores_ref[...]
    gates = scores / jnp.sum(scores, axis=0, keepdims=True)
    meta[...] = jnp.zeros_like(meta)
    meta[0:top] = ids_ref[...].astype(F32)
    meta[top : 2 * top] = gates
    go(send(meta, meta_in.at[me % 2], meta_send, meta_recv.at[me % 2], {"ep": far_inner}))
    values = x_ref[...].astype(F32)
    scale = lax.rsqrt(jnp.mean(values * values, axis=-1, keepdims=True) + 1e-06)
    normed = (values * scale * ffn_gain_ref[...]).astype(BF16)
    normed_ref[...] = normed
    parts = dense_send.shape[0]
    step_cols = deep // parts

    def cols_of(c):
        return slice(c * step_cols, (c + 1) * step_cols)

    for c in range(parts):
        go(
            send(
                normed_ref.at[:, cols_of(c)],
                dense_in.at[me % 2, :, cols_of(c)],
                dense_send.at[c],
                dense_recv.at[me % 2, c],
                {"ep": far_inner},
            )
        )
    square = (tokens, tokens)
    lane = lax.broadcasted_iota(jnp.int32, square, 1)
    sub = lax.broadcasted_iota(jnp.int32, square, 0)
    earlier = (sub < lane).astype(BF16)
    slot = lax.broadcasted_iota(jnp.int32, (capacity, tokens), 0).astype(F32)

    def route(table, first, second, at):
        named = jnp.zeros(square, F32)
        gate = jnp.zeros(square, F32)
        for n, e in enumerate((first, second)):
            place_of = e.astype(F32)
            for k in range(top):
                hit = table[k : k + 1, :] == place_of
                here = sub == n
                named = named + jnp.where(here & hit, 1.0, 0.0)
                gate = gate + jnp.where(here & hit, table[top + k : top + k + 1, :], 0.0)
        place = jnp.dot(named.astype(BF16), earlier, preferred_element_type=F32)
        for n in range(2):
            sel[2 * at + n] = jnp.where(
                slot == place[n : n + 1, :], named[n : n + 1, :], 0.0
            ).astype(BF16)
        gate_cols[at] = gate.T

    def pick(n, block):
        return jnp.dot(sel[n], block, preferred_element_type=F32).astype(BF16)

    route(meta[...], me, side, 0)
    outbound[...] = pick(1, normed)
    side_rows = go(send(outbound, rows_in.at[1], row_send, row_recv, {"ep": side}))
    rows_in[0] = pick(0, normed)

    def dense_of(q, c):
        return send(
            normed_ref.at[:, cols_of(c)],
            dense_in.at[q, :, cols_of(c)],
            dense_send.at[c],
            dense_recv.at[q, c],
            {"ep": far_inner},
        )

    def relay_of(q, c):
        return send(
            relay_out.at[q, :, cols_of(c)],
            rows_in.at[2 + q, :, cols_of(c)],
            relay_send.at[q, c],
            relay_recv.at[q, c],
            {"ep": side},
        )

    def relay(c):
        @pl.when(inner)
        def _():
            for q in range(2):
                if c == 0:
                    send(
                        meta, meta_in.at[q], meta_send, meta_recv.at[q], {"ep": far_inner}
                    ).wait_recv()
                    route(meta_in[q], me, side, 1 + q)
                dense_of(q, c).wait_recv()
                block = dense_in[q, :, cols_of(c)]
                relay_out[q, :, cols_of(c)] = pick(2 * (1 + q) + 1, block)
                relay_of(q, c).start()
                rows_in[2 + q, :, cols_of(c)] = pick(2 * (1 + q), block)

    own = pl.ds(pl.multiple_of(me * width, width), width)
    q_all[me] = q_ref[:, own]
    k_all[me] = k_ref[:, own]
    v_all[me] = v_ref[:, own]
    bias_all[me] = bias_ref[...]

    over_y, cross = {}, {}

    def forward(n):
        c, a = chunks[n]
        over_x[n].wait_recv()
        over_y[n] = go(
            send(
                fars[a].at[1, grp, c],
                fars[a].at[1, grp, c],
                y_send.at[n],
                y_recv.at[n],
                {"grp": 1 - grp},
            )
        )
        cross[0, n] = go(
            send(
                fars[a].at[1, grp, c],
                fars[a].at[2, grp, c],
                fwd_send.at[0, n],
                fwd_recv.at[0, n],
                {"tp": mates[1]},
            )
        )

    def forward_again(n):
        c, a = chunks[n]
        over_y[n].wait_recv()
        cross[1, n] = go(
            send(
                fars[a].at[1, 1 - grp, c],
                fars[a].at[2, 1 - grp, c],
                fwd_send.at[1, n],
                fwd_recv.at[1, n],
                {"tp": mates[1]},
            )
        )

    forward(0)
    for r in packs:
        for copy in packs[r]:
            copy.wait_recv()
    bias_rows[...] = bias_all[...].astype(F32)

    block = (span, span)
    key_sub = lax.broadcasted_iota(jnp.int32, block, 0)
    key_lane = lax.broadcasted_iota(jnp.int32, block, 1)
    after = (key_sub > key_lane).astype(BF16)

    def attend(i):
        def one(step, state):
            j = i - step
            past = (j * span + key_lane) < (i * span + key_sub)
            result = []
            for h in range(heads):
                total, carry = state[2 * h], state[2 * h + 1]
                cols = slice(h * head, (h + 1) * head)
                z = lax.dot_general(
                    q_all[i][:, cols],
                    k_all[j][:, cols],
                    (((1,), (1,)), ((), ())),
                    preferred_element_type=F32,
                )
                z = z * head ** (-0.5) + bias_rows[j, pl.ds(me * heads + h, 1), :]
                soft = jnp.log1p(jnp.exp(-jnp.abs(z)))
                stay = -(jnp.maximum(z, 0.0) + soft)
                stop = jnp.minimum(z, 0.0) - soft
                rest = jnp.where(past, stay, 0.0)
                hi = rest.astype(BF16)
                left = rest - hi.astype(F32)
                mid = left.astype(BF16)
                low = (left - mid.astype(F32)).astype(BF16)
                stack = jnp.concatenate([hi, mid, low], axis=0)
                sums = jnp.dot(stack, after, preferred_element_type=F32)
                within = sums[:span] + sums[span : 2 * span] + sums[2 * span :]
                local = jnp.where(past, jnp.exp(stop + within), 0.0).astype(BF16)
                part = jnp.dot(local, v_all[j][:, cols], preferred_element_type=F32)
                total = total + jnp.exp(carry) * part
                carry = carry + jnp.sum(rest, axis=1, keepdims=True)
                result += [total, carry]
            return tuple(result)

        start = (jnp.zeros((span, head), F32), jnp.zeros((span, 1), F32)) * heads
        state = lax.fori_loop(0, i + 1, one, start)
        return jnp.concatenate([state[2 * h] for h in range(heads)], axis=1).astype(BF16)

    att = {}
    forwarded = 1
    again = 0
    for r in (2, 1, 3, 0):
        dest = lax.rem(me + r, ep)
        got = attend(dest)
        if r == 0:
            att_all[me] = got
        else:
            att_send[r] = got
            att[r] = go(
                send(att_send.at[r], att_all.at[me], att_ssem.at[r], att_rsem.at[r], {"ep": dest})
            )
        if r != 1:
            forward(forwarded)
            forwarded += 1
    for copy in near:
        copy.wait_recv()
    for c in range(parts):
        relay(c)
        for _ in range(2):
            forward_again(again)
            again += 1
        for _ in range(2):
            forward(forwarded)
            forwarded += 1

    side_rows.wait_recv()

    @pl.when(jnp.logical_not(inner))
    def _():
        for q in range(2):
            for c in range(parts):
                relay_of(q, c).wait_recv()

    def hidden(g, u):
        flat = rows_in[...].reshape(ep * capacity, deep)
        gate = jnp.dot(flat, g.reshape(deep, -1), preferred_element_type=F32)
        up = jnp.dot(flat, u.reshape(deep, -1), preferred_element_type=F32)
        return (gate / (1.0 + jnp.exp(-gate)) * up).astype(BF16)

    def lower(h, d):
        return jnp.dot(h, d.reshape(-1, deep), preferred_element_type=F32)

    acc[...] = lower(hidden(g_ref[...], u_ref[...]), d_ref[...])
    acc[...] += lower(hidden(g_far[0], u_far[0]), d_far[0])
    while again < 2 * cuts:
        forward_again(again)
        again += 1
    third = hidden(g_far[1], u_far[1])
    for n in range(2 * cuts):
        cross[0, n].wait_recv()
        cross[1, n].wait_recv()
    last = hidden(g_far[2], u_far[2])
    while forwarded < len(chunks):
        forward(forwarded)
        forwarded += 1
    while again < len(chunks):
        forward_again(again)
        again += 1
    acc[...] += lower(third, d_far[1])
    for n in range(2 * cuts, len(chunks)):
        cross[0, n].wait_recv()
        cross[1, n].wait_recv()
    lowest = d_far[2].reshape(-1, deep)

    def final(r, c):
        piece = slice(r * capacity, (r + 1) * capacity)
        more = jnp.dot(last[piece], lowest[:, cols_of(c)], preferred_element_type=F32)
        return (acc[piece, cols_of(c)] + more).astype(BF16)

    def outer_of(q, c):
        return send(
            outer_out.at[q, :, cols_of(c)],
            outer_in.at[q, :, cols_of(c)],
            outer_send.at[q, c],
            outer_recv.at[q, c],
            {"ep": side},
        )

    for c in range(parts):
        for q in range(2):
            outer_out[q, :, cols_of(c)] = final(2 + q, c)

            @pl.when(jnp.logical_not(inner))
            def _():
                outer_of(q, c).start()

    for c in range(parts):
        back_out[:, cols_of(c)] = final(1, c)
    side_back = go(send(back_out, back_in.at[1], back_ssem, back_rsem, {"ep": side}))
    for c in range(parts):
        back_in[0, :, cols_of(c)] = final(0, c)

    def home_of(q, c):
        return send(
            dense_out.at[q, :, cols_of(c)],
            dense_back.at[:, cols_of(c)],
            home_send.at[q, c],
            home_recv.at[c],
            {"ep": far_base + q},
        )

    def return_home(c):
        @pl.when(inner)
        def _():
            for q in range(2):
                outer_of(q, c).wait_recv()
                mine = contract_rows(sel[2 * (1 + q)], outer_out[q, :, cols_of(c)])
                outer = contract_rows(sel[2 * (1 + q) + 1], outer_in[q, :, cols_of(c)])
                gate = gate_cols[1 + q]
                dense_out[q, :, cols_of(c)] = (
                    gate[:, 0:1] * mine + gate[:, 1:2] * outer
                ).astype(BF16)
                home_of(q, c).start()

    return_home(0)
    for r in att:
        att[r].wait_recv()
    ow_copy.wait()
    attended = jnp.concatenate([att_all[j] for j in range(ep)], axis=1)
    share = mixed_ref.shape[0]
    term = jnp.dot(attended, ow[...], preferred_element_type=F32).astype(BF16)
    proj[...] = term.reshape(proj.shape)
    shares = [
        go(send(proj.at[mates[m]], proj_in.at[m], proj_ssem.at[m], proj_rsem.at[m], {"tp": mates[m]}))
        for m in (2, 3, 1)
    ]
    for c in range(1, parts):
        return_home(c)
    whole = proj[tp].astype(F32)
    for copy in shares:
        copy.wait_recv()
    for m in (1, 2, 3):
        whole = whole + proj_in[m].astype(F32)
    scale = lax.rsqrt(jnp.mean(whole * whole, axis=-1, keepdims=True) + 1e-06)
    mixed_ref[...] = (whole * scale * mix_gain_ref[...]).astype(BF16)
    gate = gate_cols[0]
    side_back.wait_recv()
    for c in range(parts):
        mine = contract_rows(sel[0], back_in[0, :, cols_of(c)])
        beside = contract_rows(sel[1], back_in[1, :, cols_of(c)])
        acc[0:tokens, cols_of(c)] = gate[:, 0:1] * mine + gate[:, 1:2] * beside
    for c in range(parts):
        home_of(0, c).wait_recv()
        out_ref[:, cols_of(c)] = (
            acc[0:tokens, cols_of(c)] + dense_back[:, cols_of(c)].astype(F32)
        ).astype(BF16)
    for copy in started:
        copy.wait_send()
    for q in range(2):
        for c in range(parts):

            @pl.when(inner)
            def _():
                relay_of(q, c).wait_send()
                home_of(q, c).wait_send()

            @pl.when(jnp.logical_not(inner))
            def _():
                outer_of(q, c).wait_send()


def fused_device(
    groups,
    ep,
    tp,
    queries,
    keys,
    values,
    stop_bias,
    out_weight,
    mix_gain,
    moe_input,
    ffn_gain,
    expert_ids,
    expert_scores,
    gate_weight,
    up_weight,
    down_weight,
):
    span, cols = queries.shape
    tokens, deep = moe_input.shape
    top = expert_ids.shape[1]
    capacity = 3 * tokens * top // (2 * ep)
    width = cols // ep
    heads = stop_bias.shape[1]
    units = gate_weight.shape[2]
    cuts = 4
    parts = 4
    lines = 8
    gate = gate_weight.reshape(groups, cuts, deep // (groups * cuts), units)
    up = up_weight.reshape(gate.shape)
    down = down_weight.reshape(groups, cuts, units // (groups * cuts), deep)
    chunks = 3 * cuts
    vmem = pl.BlockSpec(memory_space=pltpu.VMEM)
    dma = pltpu.SemaphoreType.DMA
    return pl.pallas_call(
        functools.partial(layer_kernel, ep, capacity, cols // heads),
        out_shape=(
            jax.ShapeDtypeStruct((span // tp, deep), BF16),
            jax.ShapeDtypeStruct((tokens, deep), BF16),
        ),
        in_specs=[vmem] * 4 + [pl.BlockSpec(memory_space=pl.ANY)] + [vmem] * 8,
        out_specs=(vmem, vmem),
        scratch_shapes=[
            pltpu.VMEM((ep, span, width), BF16),
            pltpu.VMEM((ep, span, width), BF16),
            pltpu.VMEM((ep, span, width), BF16),
            pltpu.VMEM((ep, heads, span), BF16),
            pltpu.VMEM((ep, heads, span), F32),
            pltpu.VMEM((ep, span, width), BF16),
            pltpu.VMEM((ep, span, width), BF16),
            pltpu.VMEM((tp, span // tp, deep), BF16),
            pltpu.VMEM((tp, span // tp, deep), BF16),
            pltpu.VMEM(out_weight.shape, BF16),
            pltpu.VMEM((lines, tokens), F32),
            pltpu.VMEM((2, lines, tokens), F32),
            pltpu.VMEM((tokens, deep), BF16),
            pltpu.VMEM((2, tokens, deep), BF16),
            pltpu.VMEM((6, capacity, tokens), BF16),
            pltpu.VMEM((3, tokens, tokens), F32),
            pltpu.VMEM((capacity, deep), BF16),
            pltpu.VMEM((2, capacity, deep), BF16),
            pltpu.VMEM((ep, capacity, deep), BF16),
            pltpu.VMEM((ep * capacity, deep), F32),
            pltpu.VMEM((capacity, deep), BF16),
            pltpu.VMEM((2, capacity, deep), BF16),
            pltpu.VMEM((2, capacity, deep), BF16),
            pltpu.VMEM((2, capacity, deep), BF16),
            pltpu.VMEM((2, tokens, deep), BF16),
            pltpu.VMEM((tokens, deep), BF16),
            pltpu.VMEM((3,) + gate.shape, BF16),
            pltpu.VMEM((3,) + up.shape, BF16),
            pltpu.VMEM((3,) + down.shape, BF16),
            dma(()),
            dma((ep, 4)),
            dma((ep, 4)),
            dma(()),
            dma(()),
            dma(()),
            dma((2,)),
            dma((parts,)),
            dma((2, parts)),
            dma((2, parts)),
            dma((2, parts)),
            dma((ep,)),
            dma((ep,)),
            dma(()),
            dma(()),
            dma((2, parts)),
            dma((2, parts)),
            dma((2, parts)),
            dma((parts,)),
            dma((tp,)),
            dma((tp,)),
            dma((3,)),
            dma((3,)),
            dma((chunks,)),
            dma((chunks,)),
            dma((chunks,)),
            dma((chunks,)),
            dma((2, chunks)),
            dma((2, chunks)),
        ],
        compiler_params=pltpu.CompilerParams(
            collective_id=0, has_side_effects=True, vmem_limit_bytes=60 * 2**20
        ),
    )(
        queries,
        keys,
        values,
        stop_bias.T,
        out_weight,
        mix_gain.reshape(1, deep),
        moe_input,
        ffn_gain.reshape(1, deep),
        expert_ids.T,
        expert_scores.T,
        gate,
        up,
        down,
    )


def pick_plan(groups, ep, tp, *args):
    heads = args[3].shape[1]
    width = args[0].shape[1] // ep
    if groups == 2 and tp == 4 and ep == 4 and heads % ep == 0 and width % 128 == 0:
        return fused_device(groups, ep, tp, *args)
    return per_device(*args)


def solution(mesh):
    return jax.shard_map(
        functools.partial(pick_plan, mesh.shape["grp"], mesh.shape["ep"], mesh.shape["tp"]),
        mesh=mesh,
        in_specs=(
            P(("grp", "ep"), "tp"),
            P(("grp", "ep"), "tp"),
            P(("grp", "ep"), "tp"),
            P(("grp", "ep"), "tp"),
            P("tp", None),
            P(),
            P(("grp", "ep", "tp"), None),
            P(),
            P(("grp", "ep", "tp"), None),
            P(("grp", "ep", "tp"), None),
            P("ep", None, "tp"),
            P("ep", None, "tp"),
            P("ep", "tp", None),
        ),
        out_specs=(P(("grp", "ep", "tp"), None), P(("grp", "ep", "tp"), None)),
        check_vma=False,
    )
```

```python
import functools

import jax
import jax.numpy as jnp
from jax import lax
from jax.experimental import pallas as pl
from jax.experimental.pallas import tpu as pltpu
from jax.sharding import PartitionSpec as P

MESH = pl.DeviceIdType.MESH
F32 = jnp.float32
BF16 = jnp.bfloat16


def norm_rows(values, gain):
    values = values.astype(jnp.float32)
    scale = lax.rsqrt(jnp.mean(values * values, axis=-1, keepdims=True) + 1e-06)
    return values * scale * gain


def break_terms(query_heads, query_place, key_block, bias_block, first):
    span = key_block.shape[0]
    heads = query_heads.shape[1]
    key_heads = key_block.reshape(span, heads, -1)
    scores = jnp.einsum("qhd,khd->hqk", query_heads, key_heads, preferred_element_type=jnp.float32)
    scores = scores * query_heads.shape[2] ** (-0.5) + bias_block.astype(jnp.float32).T[:, None, :]
    key_place = first + jnp.arange(span)
    past = (key_place[None, :] < query_place[:, None])[None]
    rest = jnp.where(past, jax.nn.log_sigmoid(-scores), 0.0)
    later = lax.cumsum(rest, axis=2, reverse=True)
    return (scores, past, rest, later)


def block_part(scores, past, rest, later, value_block, heads):
    within = later - rest
    local = jnp.where(past, jnp.exp(jax.nn.log_sigmoid(scores) + within), 0.0).astype(jnp.bfloat16)
    span = value_block.shape[0]
    value_heads = value_block.reshape(span, heads, -1)
    part = jnp.einsum("hqk,khd->qhd", local, value_heads, preferred_element_type=jnp.float32)
    return part.reshape(part.shape[0], -1)


def keep(state):
    return state


def dispatch_plan(normed, expert_ids, experts, capacity):
    rows, top = expert_ids.shape
    flat_ids = expert_ids.reshape(rows * top)
    onehot = (flat_ids[:, None] == jnp.arange(experts)[None, :]).astype(jnp.int32)
    earlier = jnp.cumsum(onehot, axis=0) - onehot
    place = jnp.sum(earlier * onehot, axis=1)
    target = flat_ids * capacity + place
    source = (
        jnp.zeros((experts * capacity,), jnp.int32)
        .at[target]
        .set(jnp.arange(rows * top, dtype=jnp.int32) // top + 1)
    )
    padded = jnp.concatenate([jnp.zeros((1, normed.shape[1]), normed.dtype), normed], axis=0)
    return (padded[source].reshape(experts, capacity, normed.shape[1]), target)


def expert_hidden(piece, gate_weight, up_weight):
    flat = piece.reshape(-1, piece.shape[-1])
    gate = jnp.dot(flat, gate_weight[0], preferred_element_type=jnp.float32)
    upward = jnp.dot(flat, up_weight[0], preferred_element_type=jnp.float32)
    hidden = (jax.nn.silu(gate) * upward).astype(jnp.bfloat16)
    return hidden.reshape(piece.shape[0], piece.shape[1], -1)


def send_back(summed):
    return lax.all_to_all(
        summed.astype(jnp.bfloat16), "ep", split_axis=0, concat_axis=0, tiled=True
    )


def return_rows(hidden_all, down_weight, sources):
    flat = hidden_all.reshape(-1, hidden_all.shape[2])
    product = jnp.dot(flat, down_weight[0], preferred_element_type=jnp.float32)
    return send_back(
        lax.psum_scatter(
            product.reshape(sources * lax.axis_size("tp"), hidden_all.shape[1], -1).astype(
                jnp.bfloat16
            ),
            "tp",
            scatter_dimension=0,
            tiled=True,
        ).astype(jnp.float32)
    )


def per_device(
    queries,
    keys,
    values,
    stop_bias,
    out_weight,
    mix_gain,
    moe_input,
    ffn_gain,
    expert_ids,
    expert_scores,
    gate_weight,
    up_weight,
    down_weight,
):
    span = queries.shape[0]
    heads = stop_bias.shape[1]
    width_heads = queries.shape[1]
    blocks = lax.axis_size("ep")
    own_first = lax.axis_index("ep") * span
    query_heads = queries.reshape(span, heads, -1)
    query_place = own_first + jnp.arange(span)

    def piece_rows(piece, index):
        return tuple((lax.dynamic_slice_in_dim(member, index * span, span, 0) for member in piece))

    start_state = (
        jnp.zeros((blocks, heads, span), jnp.float32),
        jnp.zeros((blocks, span, width_heads), jnp.float32),
    )
    piece = (
        lax.all_gather(keys, "ep", axis=0, tiled=True),
        lax.all_gather(values, "ep", axis=0, tiled=True),
        lax.all_gather(stop_bias, "ep", axis=0, tiled=True),
    )

    def one_block(index, state):
        key_block, value_block, bias_block = piece_rows(piece, index)
        first = index * span

        def compute(inner_state):
            totals, parts = inner_state
            scores, past, rest, later = break_terms(
                query_heads, query_place, key_block, bias_block, first
            )
            part = block_part(scores, past, rest, later, value_block, heads)
            number = first // span
            totals = lax.dynamic_update_index_in_dim(totals, later[:, :, 0], number, 0)
            parts = lax.dynamic_update_index_in_dim(parts, part, number, 0)
            return (totals, parts)

        return lax.cond(first <= own_first, compute, keep, state)

    totals, parts = lax.fori_loop(0, piece[0].shape[0] // span, one_block, start_state)
    carried = lax.cumsum(totals, axis=0, reverse=True) - totals
    factor = jnp.exp(carried).transpose(0, 2, 1)[:, :, :, None]
    attended = jnp.sum(factor * parts.reshape(blocks, span, heads, -1), axis=0).reshape(
        span, width_heads
    )
    attended = attended.astype(jnp.bfloat16)
    projected = lax.psum_scatter(
        jnp.dot(attended, out_weight, preferred_element_type=jnp.float32).astype(jnp.bfloat16),
        "tp",
        scatter_dimension=0,
        tiled=True,
    ).astype(jnp.float32)
    mixed = norm_rows(projected, mix_gain).astype(jnp.bfloat16)
    normed = norm_rows(moe_input, ffn_gain).astype(jnp.bfloat16)
    rows, top = expert_ids.shape
    experts = lax.axis_size("ep")
    capacity = 3 * rows * top // (2 * experts)
    weights = expert_scores / jnp.sum(expert_scores, axis=1, keepdims=True)
    outbound, target = dispatch_plan(normed, expert_ids, experts, capacity)
    arrived = lax.all_to_all(outbound, "ep", split_axis=0, concat_axis=0, tiled=True)
    hidden_all = expert_hidden(
        lax.all_gather(arrived, "tp", axis=0, tiled=True), gate_weight, up_weight
    )
    returned = return_rows(hidden_all, down_weight, arrived.shape[0])
    picked = returned.reshape(experts * capacity, -1)[target].reshape(rows, top, -1)
    experts_mixed = jnp.sum(picked.astype(jnp.float32) * weights[:, :, None], axis=1).astype(
        jnp.bfloat16
    )
    return (mixed, experts_mixed)


def contract_rows(left, right):
    return lax.dot_general(left, right, (((0,), (0,)), ((), ())), preferred_element_type=F32)


def layer_kernel(
    ep,
    capacity,
    head,
    q_ref,
    k_ref,
    v_ref,
    bias_ref,
    ow_ref,
    mix_gain_ref,
    x_ref,
    ffn_gain_ref,
    ids_ref,
    scores_ref,
    g_ref,
    u_ref,
    d_ref,
    mixed_ref,
    out_ref,
    q_all,
    k_all,
    v_all,
    bias_all,
    bias_rows,
    att_send,
    att_all,
    proj,
    proj_in,
    ow,
    meta,
    meta_in,
    normed_ref,
    dense_in,
    sel,
    gate_cols,
    outbound,
    relay_out,
    rows_in,
    acc,
    back_out,
    back_in,
    outer_out,
    outer_in,
    dense_out,
    dense_back,
    g_far,
    u_far,
    d_far,
    ow_sem,
    pack_send,
    pack_recv,
    row_send,
    row_recv,
    meta_send,
    meta_recv,
    dense_send,
    dense_recv,
    relay_send,
    relay_recv,
    att_ssem,
    att_rsem,
    back_ssem,
    back_rsem,
    outer_send,
    outer_recv,
    home_send,
    home_recv,
    proj_ssem,
    proj_rsem,
    near_send,
    near_recv,
    x_send,
    x_recv,
    y_send,
    y_recv,
    fwd_send,
    fwd_recv,
):
    me = lax.axis_index("ep")
    tp = lax.axis_index("tp")
    grp = lax.axis_index("grp")
    chip, core = tp // 2, tp % 2
    mates = [None, chip * 2 + (1 - core), (1 - chip) * 2 + core, (1 - chip) * 2 + (1 - core)]
    span = q_ref.shape[0]
    width = q_all.shape[2]
    heads = width // head

    half = me // 2
    inner = lax.rem(me + 1, ep) >= 2
    side = me + 1 - 2 * (me % 2)
    far_inner = 2 - half
    far_base = 2 * (1 - half)
    ow_copy = pltpu.make_async_copy(ow_ref, ow, ow_sem)
    ow_copy.start()

    barrier = pltpu.get_barrier_semaphore()
    peers = [{"ep": lax.rem(me + r, ep)} for r in range(1, ep)]
    peers += [{"tp": mates[m]} for m in (1, 2, 3)] + [{"grp": 1 - grp}]
    for peer in peers:
        pl.semaphore_signal(barrier, inc=1, device_id=peer, device_id_type=MESH)
    pl.semaphore_wait(barrier, len(peers))

    def send(src, dst, ssem, rsem, peer):
        return pltpu.make_async_remote_copy(
            src_ref=src,
            dst_ref=dst,
            send_sem=ssem,
            recv_sem=rsem,
            device_id=peer,
            device_id_type=MESH,
        )

    weights = (g_ref, u_ref, d_ref)
    fars = (g_far, u_far, d_far)
    started = []

    def go(copy):
        copy.start()
        started.append(copy)
        return copy

    cuts = g_ref.shape[1]
    chunks = [(c, a) for c in range(cuts) for a in range(2)] + [(c, 2) for c in range(cuts)]
    over_x = {}
    for n, (c, a) in enumerate(chunks):
        over_x[n] = go(
            send(
                weights[a].at[grp, c],
                fars[a].at[1, grp, c],
                x_send.at[n],
                x_recv.at[n],
                {"tp": mates[2]},
            )
        )
    near = [
        go(
            send(
                weights[a], fars[a].at[0], near_send.at[a], near_recv.at[a], {"tp": mates[1]}
            )
        )
        for a in range(3)
    ]
    tokens, deep = x_ref.shape
    top = ids_ref.shape[0]
    scores = scores_ref[...]
    gates = scores / jnp.sum(scores, axis=0, keepdims=True)
    meta[...] = jnp.zeros_like(meta)
    meta[0:top] = ids_ref[...].astype(F32)
    meta[top : 2 * top] = gates
    go(send(meta, meta_in.at[me % 2], meta_send, meta_recv.at[me % 2], {"ep": far_inner}))
    values = x_ref[...].astype(F32)
    scale = lax.rsqrt(jnp.mean(values * values, axis=-1, keepdims=True) + 1e-06)
    normed = (values * scale * ffn_gain_ref[...]).astype(BF16)
    normed_ref[...] = normed
    parts = dense_send.shape[0]
    step_cols = deep // parts

    def cols_of(c):
        return slice(c * step_cols, (c + 1) * step_cols)

    for c in range(parts):
        go(
            send(
                normed_ref.at[:, cols_of(c)],
                dense_in.at[me % 2, :, cols_of(c)],
                dense_send.at[c],
                dense_recv.at[me % 2, c],
                {"ep": far_inner},
            )
        )
    square = (tokens, tokens)
    lane = lax.broadcasted_iota(jnp.int32, square, 1)
    sub = lax.broadcasted_iota(jnp.int32, square, 0)
    earlier = (sub < lane).astype(BF16)
    slot = lax.broadcasted_iota(jnp.int32, (capacity, tokens), 0).astype(F32)

    def route(table, first, second, at):
        named = jnp.zeros(square, F32)
        gate = jnp.zeros(square, F32)
        for n, e in enumerate((first, second)):
            place_of = e.astype(F32)
            for k in range(top):
                hit = table[k : k + 1, :] == place_of
                here = sub == n
                named = named + jnp.where(here & hit, 1.0, 0.0)
                gate = gate + jnp.where(here & hit, table[top + k : top + k + 1, :], 0.0)
        place = jnp.dot(named.astype(BF16), earlier, preferred_element_type=F32)
        for n in range(2):
            sel[2 * at + n] = jnp.where(
                slot == place[n : n + 1, :], named[n : n + 1, :], 0.0
            ).astype(BF16)
        gate_cols[at] = gate.T

    def pick(n, block):
        return jnp.dot(sel[n], block, preferred_element_type=F32).astype(BF16)

    route(meta[...], me, side, 0)
    outbound[...] = pick(1, normed)
    side_rows = go(send(outbound, rows_in.at[1], row_send, row_recv, {"ep": side}))
    rows_in[0] = pick(0, normed)

    def dense_of(q, c):
        return send(
            normed_ref.at[:, cols_of(c)],
            dense_in.at[q, :, cols_of(c)],
            dense_send.at[c],
            dense_recv.at[q, c],
            {"ep": far_inner},
        )

    def relay_of(q, c):
        return send(
            relay_out.at[q, :, cols_of(c)],
            rows_in.at[2 + q, :, cols_of(c)],
            relay_send.at[q, c],
            relay_recv.at[q, c],
            {"ep": side},
        )

    def relay(c):
        @pl.when(inner)
        def _():
            for q in range(2):
                if c == 0:
                    send(
                        meta, meta_in.at[q], meta_send, meta_recv.at[q], {"ep": far_inner}
                    ).wait_recv()
                    route(meta_in[q], me, side, 1 + q)
                dense_of(q, c).wait_recv()
                block = dense_in[q, :, cols_of(c)]
                relay_out[q, :, cols_of(c)] = pick(2 * (1 + q) + 1, block)
                relay_of(q, c).start()
                rows_in[2 + q, :, cols_of(c)] = pick(2 * (1 + q), block)

    packs = {}
    for r in (2, 1, 3)[: ep - 1]:
        dest = lax.rem(me + r, ep)
        cols = pl.ds(pl.multiple_of(dest * width, width), width)
        pieces = (
            (q_ref.at[:, cols], q_all.at[me]),
            (k_ref.at[:, cols], k_all.at[me]),
            (v_ref.at[:, cols], v_all.at[me]),
            (bias_ref, bias_all.at[me]),
        )
        packs[r] = [
            go(send(s, t, pack_send.at[r, n], pack_recv.at[r, n], {"ep": dest}))
            for n, (s, t) in enumerate(pieces)
        ]
    own = pl.ds(pl.multiple_of(me * width, width), width)
    q_all[me] = q_ref[:, own]
    k_all[me] = k_ref[:, own]
    v_all[me] = v_ref[:, own]
    bias_all[me] = bias_ref[...]

    over_y, cross = {}, {}

    def forward(n):
        c, a = chunks[n]
        over_x[n].wait_recv()
        over_y[n] = go(
            send(
                fars[a].at[1, grp, c],
                fars[a].at[1, grp, c],
                y_send.at[n],
                y_recv.at[n],
                {"grp": 1 - grp},
            )
        )
        cross[0, n] = go(
            send(
                fars[a].at[1, grp, c],
                fars[a].at[2, grp, c],
                fwd_send.at[0, n],
                fwd_recv.at[0, n],
                {"tp": mates[1]},
            )
        )

    def forward_again(n):
        c, a = chunks[n]
        over_y[n].wait_recv()
        cross[1, n] = go(
            send(
                fars[a].at[1, 1 - grp, c],
                fars[a].at[2, 1 - grp, c],
                fwd_send.at[1, n],
                fwd_recv.at[1, n],
                {"tp": mates[1]},
            )
        )

    block = (span, span)
    key_sub = lax.broadcasted_iota(jnp.int32, block, 0)
    key_lane = lax.broadcasted_iota(jnp.int32, block, 1)
    after = (key_sub > key_lane).astype(BF16)

    def attend(i):
        def one(step, state):
            j = i - step
            past = (j * span + key_lane) < (i * span + key_sub)
            result = []
            for h in range(heads):
                total, carry = state[2 * h], state[2 * h + 1]
                cols = slice(h * head, (h + 1) * head)
                z = lax.dot_general(
                    q_all[i][:, cols],
                    k_all[j][:, cols],
                    (((1,), (1,)), ((), ())),
                    preferred_element_type=F32,
                )
                z = z * head ** (-0.5) + bias_rows[j, pl.ds(me * heads + h, 1), :]
                soft = jnp.log1p(jnp.exp(-jnp.abs(z)))
                stay = -(jnp.maximum(z, 0.0) + soft)
                stop = jnp.minimum(z, 0.0) - soft
                rest = jnp.where(past, stay, 0.0)
                hi = rest.astype(BF16)
                left = rest - hi.astype(F32)
                mid = left.astype(BF16)
                low = (left - mid.astype(F32)).astype(BF16)
                stack = jnp.concatenate([hi, mid, low], axis=0)
                sums = jnp.dot(stack, after, preferred_element_type=F32)
                within = sums[:span] + sums[span : 2 * span] + sums[2 * span :]
                local = jnp.where(past, jnp.exp(stop + within), 0.0).astype(BF16)
                part = jnp.dot(local, v_all[j][:, cols], preferred_element_type=F32)
                total = total + jnp.exp(carry) * part
                carry = carry + jnp.sum(rest, axis=1, keepdims=True)
                result += [total, carry]
            return tuple(result)

        start = (jnp.zeros((span, head), F32), jnp.zeros((span, 1), F32)) * heads
        state = lax.fori_loop(0, i + 1, one, start)
        return jnp.concatenate([state[2 * h] for h in range(heads)], axis=1).astype(BF16)

    for copy in near:
        copy.wait_recv()
    again = forwarded = 0
    for c in range(parts):
        for _ in range(2):
            forward(forwarded)
            forwarded += 1
        relay(c)
        for _ in range(2 if c else 0):
            forward_again(again)
            again += 1

    side_rows.wait_recv()

    @pl.when(jnp.logical_not(inner))
    def _():
        for q in range(2):
            for c in range(parts):
                relay_of(q, c).wait_recv()

    def hidden(g, u):
        flat = rows_in[...].reshape(ep * capacity, deep)
        gate = jnp.dot(flat, g.reshape(deep, -1), preferred_element_type=F32)
        up = jnp.dot(flat, u.reshape(deep, -1), preferred_element_type=F32)
        return (gate / (1.0 + jnp.exp(-gate)) * up).astype(BF16)

    def lower(h, d):
        return jnp.dot(h, d.reshape(-1, deep), preferred_element_type=F32)

    acc[...] = lower(hidden(g_ref[...], u_ref[...]), d_ref[...])
    for _ in range(2):
        forward_again(again)
        again += 1
        forward(forwarded)
        forwarded += 1
    acc[...] += lower(hidden(g_far[0], u_far[0]), d_far[0])
    for r in packs:
        for copy in packs[r]:
            copy.wait_recv()
    bias_rows[...] = bias_all[...].astype(F32)

    att = {}
    for r in (2, 1, 3, 0):
        dest = lax.rem(me + r, ep)
        got = attend(dest)
        if r == 0:
            att_all[me] = got
        else:
            att_send[r] = got
            att[r] = go(
                send(att_send.at[r], att_all.at[me], att_ssem.at[r], att_rsem.at[r], {"ep": dest})
            )
        if forwarded < len(chunks):
            forward(forwarded)
            forwarded += 1
        forward_again(again)
        again += 1
    third = hidden(g_far[1], u_far[1])
    for n in range(2 * cuts):
        cross[0, n].wait_recv()
        cross[1, n].wait_recv()
    last = hidden(g_far[2], u_far[2])
    while forwarded < len(chunks):
        forward(forwarded)
        forwarded += 1
    while again < len(chunks):
        forward_again(again)
        again += 1
    acc[...] += lower(third, d_far[1])
    for n in range(2 * cuts, len(chunks)):
        cross[0, n].wait_recv()
        cross[1, n].wait_recv()
    lowest = d_far[2].reshape(-1, deep)

    def final(r, c):
        piece = slice(r * capacity, (r + 1) * capacity)
        more = jnp.dot(last[piece], lowest[:, cols_of(c)], preferred_element_type=F32)
        return (acc[piece, cols_of(c)] + more).astype(BF16)

    def outer_of(q, c):
        return send(
            outer_out.at[q, :, cols_of(c)],
            outer_in.at[q, :, cols_of(c)],
            outer_send.at[q, c],
            outer_recv.at[q, c],
            {"ep": side},
        )

    for c in range(parts):
        for q in range(2):
            outer_out[q, :, cols_of(c)] = final(2 + q, c)

            @pl.when(jnp.logical_not(inner))
            def _():
                outer_of(q, c).start()

    for c in range(parts):
        back_out[:, cols_of(c)] = final(1, c)
    side_back = go(send(back_out, back_in.at[1], back_ssem, back_rsem, {"ep": side}))
    for c in range(parts):
        back_in[0, :, cols_of(c)] = final(0, c)

    def home_of(q, c):
        return send(
            dense_out.at[q, :, cols_of(c)],
            dense_back.at[:, cols_of(c)],
            home_send.at[q, c],
            home_recv.at[c],
            {"ep": far_base + q},
        )

    def return_home(c):
        @pl.when(inner)
        def _():
            for q in range(2):
                outer_of(q, c).wait_recv()
                mine = contract_rows(sel[2 * (1 + q)], outer_out[q, :, cols_of(c)])
                outer = contract_rows(sel[2 * (1 + q) + 1], outer_in[q, :, cols_of(c)])
                gate = gate_cols[1 + q]
                dense_out[q, :, cols_of(c)] = (
                    gate[:, 0:1] * mine + gate[:, 1:2] * outer
                ).astype(BF16)
                home_of(q, c).start()

    return_home(0)
    for r in att:
        att[r].wait_recv()
    ow_copy.wait()
    attended = jnp.concatenate([att_all[j] for j in range(ep)], axis=1)
    share = mixed_ref.shape[0]
    term = jnp.dot(attended, ow[...], preferred_element_type=F32).astype(BF16)
    proj[...] = term.reshape(proj.shape)
    shares = [
        go(send(proj.at[mates[m]], proj_in.at[m], proj_ssem.at[m], proj_rsem.at[m], {"tp": mates[m]}))
        for m in (2, 3, 1)
    ]
    for c in range(1, parts):
        return_home(c)
    whole = proj[tp].astype(F32)
    for copy in shares:
        copy.wait_recv()
    for m in (1, 2, 3):
        whole = whole + proj_in[m].astype(F32)
    scale = lax.rsqrt(jnp.mean(whole * whole, axis=-1, keepdims=True) + 1e-06)
    mixed_ref[...] = (whole * scale * mix_gain_ref[...]).astype(BF16)
    gate = gate_cols[0]
    side_back.wait_recv()
    for c in range(parts):
        mine = contract_rows(sel[0], back_in[0, :, cols_of(c)])
        beside = contract_rows(sel[1], back_in[1, :, cols_of(c)])
        acc[0:tokens, cols_of(c)] = gate[:, 0:1] * mine + gate[:, 1:2] * beside
    for c in range(parts):
        home_of(0, c).wait_recv()
        out_ref[:, cols_of(c)] = (
            acc[0:tokens, cols_of(c)] + dense_back[:, cols_of(c)].astype(F32)
        ).astype(BF16)
    for copy in started:
        copy.wait_send()
    for q in range(2):
        for c in range(parts):

            @pl.when(inner)
            def _():
                relay_of(q, c).wait_send()
                home_of(q, c).wait_send()

            @pl.when(jnp.logical_not(inner))
            def _():
                outer_of(q, c).wait_send()


def settle_kernel(mixed_ref, out_ref, mixed_to, out_to):
    mixed_to[...] = mixed_ref[...]
    out_to[...] = out_ref[...]


def fused_device(
    groups,
    ep,
    tp,
    queries,
    keys,
    values,
    stop_bias,
    out_weight,
    mix_gain,
    moe_input,
    ffn_gain,
    expert_ids,
    expert_scores,
    gate_weight,
    up_weight,
    down_weight,
):
    span, cols = queries.shape
    tokens, deep = moe_input.shape
    top = expert_ids.shape[1]
    capacity = 3 * tokens * top // (2 * ep)
    width = cols // ep
    heads = stop_bias.shape[1]
    units = gate_weight.shape[2]
    cuts = 4
    parts = 4
    lines = 8
    gate = gate_weight.reshape(groups, cuts, deep // (groups * cuts), units)
    up = up_weight.reshape(gate.shape)
    down = down_weight.reshape(groups, cuts, units // (groups * cuts), deep)
    chunks = 3 * cuts
    vmem = pl.BlockSpec(memory_space=pltpu.VMEM)
    dma = pltpu.SemaphoreType.DMA
    results = pl.pallas_call(
        functools.partial(layer_kernel, ep, capacity, cols // heads),
        out_shape=(
            jax.ShapeDtypeStruct((span // tp, deep), BF16),
            jax.ShapeDtypeStruct((tokens, deep), BF16),
        ),
        in_specs=[vmem] * 4 + [pl.BlockSpec(memory_space=pl.ANY)] + [vmem] * 8,
        out_specs=(vmem, vmem),
        scratch_shapes=[
            pltpu.VMEM((ep, span, width), BF16),
            pltpu.VMEM((ep, span, width), BF16),
            pltpu.VMEM((ep, span, width), BF16),
            pltpu.VMEM((ep, heads, span), BF16),
            pltpu.VMEM((ep, heads, span), F32),
            pltpu.VMEM((ep, span, width), BF16),
            pltpu.VMEM((ep, span, width), BF16),
            pltpu.VMEM((tp, span // tp, deep), BF16),
            pltpu.VMEM((tp, span // tp, deep), BF16),
            pltpu.VMEM(out_weight.shape, BF16),
            pltpu.VMEM((lines, tokens), F32),
            pltpu.VMEM((2, lines, tokens), F32),
            pltpu.VMEM((tokens, deep), BF16),
            pltpu.VMEM((2, tokens, deep), BF16),
            pltpu.VMEM((6, capacity, tokens), BF16),
            pltpu.VMEM((3, tokens, tokens), F32),
            pltpu.VMEM((capacity, deep), BF16),
            pltpu.VMEM((2, capacity, deep), BF16),
            pltpu.VMEM((ep, capacity, deep), BF16),
            pltpu.VMEM((ep * capacity, deep), F32),
            pltpu.VMEM((capacity, deep), BF16),
            pltpu.VMEM((2, capacity, deep), BF16),
            pltpu.VMEM((2, capacity, deep), BF16),
            pltpu.VMEM((2, capacity, deep), BF16),
            pltpu.VMEM((2, tokens, deep), BF16),
            pltpu.VMEM((tokens, deep), BF16),
            pltpu.VMEM((3,) + gate.shape, BF16),
            pltpu.VMEM((3,) + up.shape, BF16),
            pltpu.VMEM((3,) + down.shape, BF16),
            dma(()),
            dma((ep, 4)),
            dma((ep, 4)),
            dma(()),
            dma(()),
            dma(()),
            dma((2,)),
            dma((parts,)),
            dma((2, parts)),
            dma((2, parts)),
            dma((2, parts)),
            dma((ep,)),
            dma((ep,)),
            dma(()),
            dma(()),
            dma((2, parts)),
            dma((2, parts)),
            dma((2, parts)),
            dma((parts,)),
            dma((tp,)),
            dma((tp,)),
            dma((3,)),
            dma((3,)),
            dma((chunks,)),
            dma((chunks,)),
            dma((chunks,)),
            dma((chunks,)),
            dma((2, chunks)),
            dma((2, chunks)),
        ],
        compiler_params=pltpu.CompilerParams(
            collective_id=0, has_side_effects=True, vmem_limit_bytes=60 * 2**20
        ),
    )(
        queries,
        keys,
        values,
        stop_bias.T,
        out_weight,
        mix_gain.reshape(1, deep),
        moe_input,
        ffn_gain.reshape(1, deep),
        expert_ids.T,
        expert_scores.T,
        gate,
        up,
        down,
    )
    return pl.pallas_call(
        settle_kernel,
        out_shape=tuple(jax.ShapeDtypeStruct(r.shape, r.dtype) for r in results),
        in_specs=[vmem] * 2,
        out_specs=(vmem, vmem),
    )(*results)


def pick_plan(groups, ep, tp, *args):
    heads = args[3].shape[1]
    width = args[0].shape[1] // ep
    if groups == 2 and tp == 4 and ep == 4 and heads % ep == 0 and width % 128 == 0:
        return fused_device(groups, ep, tp, *args)
    return per_device(*args)


def solution(mesh):
    return jax.shard_map(
        functools.partial(pick_plan, mesh.shape["grp"], mesh.shape["ep"], mesh.shape["tp"]),
        mesh=mesh,
        in_specs=(
            P(("grp", "ep"), "tp"),
            P(("grp", "ep"), "tp"),
            P(("grp", "ep"), "tp"),
            P(("grp", "ep"), "tp"),
            P("tp", None),
            P(),
            P(("grp", "ep", "tp"), None),
            P(),
            P(("grp", "ep", "tp"), None),
            P(("grp", "ep", "tp"), None),
            P("ep", None, "tp"),
            P("ep", None, "tp"),
            P("ep", "tp", None),
        ),
        out_specs=(P(("grp", "ep", "tp"), None), P(("grp", "ep", "tp"), None)),
        check_vma=False,
    )
```
